32 devices in a mesh: fs: 4 (over z), tp: 4 (over y, x), rep: 2 (over core).
Axes of the slice: x: 2, y: 2, z: 4, core: 2. Of those that a mesh axis runs over, the one named last changes fastest.
Arguments:
- gate_weight: float32 [2048, 5632], P('fs', 'tp'), may hold values from -6 to 6
- gate_momentum: float32 [2048, 5632], P('fs', 'tp'), may hold values from -60 to 60
- gate_grads: float32 [2, 2048, 5632], P('rep', 'fs', 'tp'), may hold values from -3500 to 3500
- gate_rows: float32 [2048], P('fs'), may hold values from 0.3 to 3
- gate_columns: float32 [5632], P('tp'), may hold values from 0.3 to 3
- up_weight: float32 [2048, 5632], P('fs', 'tp'), may hold values from -6 to 6
- up_momentum: float32 [2048, 5632], P('fs', 'tp'), may hold values from -60 to 60
- up_grads: float32 [2, 2048, 5632], P('rep', 'fs', 'tp'), may hold values from -3500 to 3500
- up_rows: float32 [2048], P('fs'), may hold values from 0.3 to 3
- up_columns: float32 [5632], P('tp'), may hold values from 0.3 to 3
- down_weight: float32 [5632, 2048], P('fs', 'tp'), may hold values from -6 to 6
- down_momentum: float32 [5632, 2048], P('fs', 'tp'), may hold values from -60 to 60
- down_grads: float32 [2, 5632, 2048], P('rep', 'fs', 'tp'), may hold values from -3500 to 3500
- down_rows: float32 [5632], P('fs'), may hold values from 0.3 to 3
- down_columns: float32 [2048], P('tp'), may hold values from 0.3 to 3
- mixer_weight: float32 [2048, 2048], P('fs', 'tp'), may hold values from -6 to 6
- mixer_momentum: float32 [2048, 2048], P('fs', 'tp'), may hold values from -60 to 60
- mixer_grads: float32 [2, 2048, 2048], P('rep', 'fs', 'tp'), may hold values from -3500 to 3500
- mixer_rows: float32 [2048], P('fs'), may hold values from 0.3 to 3
- mixer_columns: float32 [2048], P('tp'), may hold values from 0.3 to 3
Outputs:
- gate_weight_next: float32 [2048, 5632], P('fs', 'tp')
- gate_momentum_next: float32 [2048, 5632], P('fs', 'tp')
- gate_rows_next: float32 [2048], P('fs')
- gate_columns_next: float32 [5632], P('tp')
- up_weight_next: float32 [2048, 5632], P('fs', 'tp')
- up_momentum_next: float32 [2048, 5632], P('fs', 'tp')
- up_rows_next: float32 [2048], P('fs')
- up_columns_next: float32 [5632], P('tp')
- down_weight_next: float32 [5632, 2048], P('fs', 'tp')
- down_momentum_next: float32 [5632, 2048], P('fs', 'tp')
- down_rows_next: float32 [5632], P('fs')
- down_columns_next: float32 [2048], P('tp')
- mixer_weight_next: float32 [2048, 2048], P('fs', 'tp')
- mixer_momentum_next: float32 [2048, 2048], P('fs', 'tp')
- mixer_rows_next: float32 [2048], P('fs')
- mixer_columns_next: float32 [2048], P('tp')
The draws below stay inside these ranges and needn't reach their ends.
All inputs are finite; a program needn't handle non-finite values.
Results may differ from the reference program's by a relative error of at most 0.00002.
Values sent between devices are 32-bit elements; how exact they have to be, the bound alone decides.
A program may use at most 128 MiB of HBM per device.

```python
import math
import jax
import jax.numpy as jnp
from jax import lax

D = 2048
FF = 5632
N_REP = 2


def grad_draw(key, salt, height, width):
    base_key = jax.random.fold_in(key, salt)
    keys = jax.random.split(base_key, 5)
    entry_scale = 10.0 ** jax.random.uniform(keys[4], (height, width), jnp.float32, -1.0, 1.0)
    row_scale = 10.0 ** jax.random.uniform(keys[0], (height,), jnp.float32, -0.5, 0.5)
    col_scale = 10.0 ** jax.random.uniform(keys[1], (width,), jnp.float32, -0.5, 0.5)
    values = jnp.clip(jax.random.normal(keys[2], (N_REP, height, width), jnp.float32), -6.0, 6.0)
    row_trend = 3.0 ** (jnp.arange(height, dtype=jnp.float32) / height - 0.5)
    col_trend = 3.0 ** (jnp.arange(width, dtype=jnp.float32) / width - 0.5)
    scales = (row_scale * row_trend)[:, None] * (col_scale * col_trend)[None, :] * entry_scale
    return values * scales[None, :, :]


def momentum_draw(key, salt, height, width):
    base_key = jax.random.fold_in(key, salt)
    keys = jax.random.split(base_key, 2)
    entry_scale = 10.0 ** jax.random.uniform(keys[0], (height, width), jnp.float32, -1.0, 1.0)
    values = jnp.clip(jax.random.normal(keys[1], (height, width), jnp.float32), -6.0, 6.0)
    return values * entry_scale


def draw_gate_grads(key, part):
    return grad_draw(key, 11, D, FF)


def draw_up_grads(key, part):
    return grad_draw(key, 12, D, FF)


def draw_down_grads(key, part):
    return grad_draw(key, 13, FF, D)


def draw_mixer_grads(key, part):
    return grad_draw(key, 14, D, D)


def draw_gate_momentum(key, part):
    return momentum_draw(key, 21, D, FF)


def draw_up_momentum(key, part):
    return momentum_draw(key, 22, D, FF)


def draw_down_momentum(key, part):
    return momentum_draw(key, 23, FF, D)


def draw_mixer_momentum(key, part):
    return momentum_draw(key, 24, D, D)


def level_of(own_key, extent, cuts, least, largest):
    level, own = 1.0, jax.random.fold_in(own_key, 6)
    for axis_at, blocks in cuts:
        steps = jnp.exp(jax.random.uniform(jax.random.fold_in(own, axis_at), (blocks,), jnp.float32, least / len(cuts), largest / len(cuts)))
        level = level * jnp.repeat(steps, extent[axis_at] // blocks).reshape([-1 if axis == axis_at else 1 for axis in range(len(extent))])
    return level


def centred(own_key, extent, scale, most, cuts=(), held_as=jnp.bfloat16):
    loudness = level_of(own_key, extent, cuts, -0.22, 0.18) if cuts else 1.0
    entries = jax.random.normal(own_key, extent, jnp.float32) * scale * loudness
    return jnp.minimum(jnp.maximum(entries, -most), most).astype(held_as)


def setup_inputs(seed: int = 0) -> dict:
    key_of = jax.random.split(jax.random.key(seed), 21)
    gate_weight = centred(key_of[0], (D, FF), 1.0, 6.0, ((0, 4), (1, 4)), jnp.float32)
    gate_momentum = draw_gate_momentum(jax.random.fold_in(key_of[20], 71), 0)
    gate_grads = draw_gate_grads(jax.random.fold_in(key_of[20], 71), 0)
    gate_rows = jnp.clip(jnp.exp(math.log(3.0) - 2.3025851 * jax.random.uniform(key_of[3], (D,), jnp.float32) ** level_of(key_of[3], (D,), ((0, 4),), -0.2, 0.2)), 0.3, 3.0)
    gate_columns = jnp.clip(jnp.exp(math.log(3.0) - 2.3025851 * jax.random.uniform(key_of[4], (FF,), jnp.float32) ** level_of(key_of[4], (FF,), ((0, 4),), -0.2, 0.2)), 0.3, 3.0)
    up_weight = centred(key_of[5], (D, FF), 1.0, 6.0, ((0, 4), (1, 4)), jnp.float32)
    up_momentum = draw_up_momentum(jax.random.fold_in(key_of[20], 71), 0)
    up_grads = draw_up_grads(jax.random.fold_in(key_of[20], 71), 0)
    up_rows = jnp.clip(jnp.exp(math.log(3.0) - 2.3025851 * jax.random.uniform(key_of[8], (D,), jnp.float32) ** level_of(key_of[8], (D,), ((0, 4),), -0.2, 0.2)), 0.3, 3.0)
    up_columns = jnp.clip(jnp.exp(math.log(3.0) - 2.3025851 * jax.random.uniform(key_of[9], (FF,), jnp.float32) ** level_of(key_of[9], (FF,), ((0, 4),), -0.2, 0.2)), 0.3, 3.0)
    down_weight = centred(key_of[10], (FF, D), 1.0, 6.0, ((0, 4), (1, 4)), jnp.float32)
    down_momentum = draw_down_momentum(jax.random.fold_in(key_of[20], 71), 0)
    down_grads = draw_down_grads(jax.random.fold_in(key_of[20], 71), 0)
    down_rows = jnp.clip(jnp.exp(math.log(3.0) - 2.3025851 * jax.random.uniform(key_of[13], (FF,), jnp.float32) ** level_of(key_of[13], (FF,), ((0, 4),), -0.2, 0.2)), 0.3, 3.0)
    down_columns = jnp.clip(jnp.exp(math.log(3.0) - 2.3025851 * jax.random.uniform(key_of[14], (D,), jnp.float32) ** level_of(key_of[14], (D,), ((0, 4),), -0.2, 0.2)), 0.3, 3.0)
    mixer_weight = centred(key_of[15], (D, D), 1.0, 6.0, ((0, 4), (1, 4)), jnp.float32)
    mixer_momentum = draw_mixer_momentum(jax.random.fold_in(key_of[20], 71), 0)
    mixer_grads = draw_mixer_grads(jax.random.fold_in(key_of[20], 71), 0)
    mixer_rows = jnp.clip(jnp.exp(math.log(3.0) - 2.3025851 * jax.random.uniform(key_of[18], (D,), jnp.float32) ** level_of(key_of[18], (D,), ((0, 4),), -0.2, 0.2)), 0.3, 3.0)
    mixer_columns = jnp.clip(jnp.exp(math.log(3.0) - 2.3025851 * jax.random.uniform(key_of[19], (D,), jnp.float32) ** level_of(key_of[19], (D,), ((0, 4),), -0.2, 0.2)), 0.3, 3.0)
    return {"gate_weight": gate_weight, "gate_momentum": gate_momentum, "gate_grads": gate_grads, "gate_rows": gate_rows, "gate_columns": gate_columns, "up_weight": up_weight, "up_momentum": up_momentum, "up_grads": up_grads, "up_rows": up_rows, "up_columns": up_columns, "down_weight": down_weight, "down_momentum": down_momentum, "down_grads": down_grads, "down_rows": down_rows, "down_columns": down_columns, "mixer_weight": mixer_weight, "mixer_momentum": mixer_momentum, "mixer_grads": mixer_grads, "mixer_rows": mixer_rows, "mixer_columns": mixer_columns}


momentum_decay = 0.9
moment_decay = 0.95
clip_level = 0.25
step_rate = 0.1

def update_matrix(weight, momentum, grads, rows, columns):
    grad = lax.optimization_barrier(jnp.sum(grads.astype(jnp.float32), axis=0))
    momentum_next = momentum_decay * momentum + (1.0 - momentum_decay) * grad
    squares = grad * grad
    rows_next = moment_decay * rows + (1.0 - moment_decay) * lax.optimization_barrier(jnp.mean(squares, axis=1))
    columns_next = moment_decay * columns + (1.0 - moment_decay) * lax.optimization_barrier(jnp.mean(squares, axis=0))
    row_mean = jnp.mean(rows_next)
    update = momentum_next * lax.rsqrt(rows_next[:, None] * columns_next[None, :] / row_mean)
    spread = jnp.sqrt(jnp.mean(update * update))
    factor = jnp.maximum(1.0, spread / clip_level)
    weight_next = weight - step_rate * update / factor
    return (weight_next, momentum_next, rows_next, columns_next)

def reference(gate_weight, gate_momentum, gate_grads, gate_rows, gate_columns, up_weight, up_momentum, up_grads, up_rows, up_columns, down_weight, down_momentum, down_grads, down_rows, down_columns, mixer_weight, mixer_momentum, mixer_grads, mixer_rows, mixer_columns):
    first = update_matrix(gate_weight, gate_momentum, gate_grads, gate_rows, gate_columns)
    second = update_matrix(up_weight, up_momentum, up_grads, up_rows, up_columns)
    third = update_matrix(down_weight, down_momentum, down_grads, down_rows, down_columns)
    fourth = update_matrix(mixer_weight, mixer_momentum, mixer_grads, mixer_rows, mixer_columns)
    return (first[0], first[1], first[2], first[3], second[0], second[1], second[2], second[3], third[0], third[1], third[2], third[3], fourth[0], fourth[1], fourth[2], fourth[3])
```

```python
import functools
import math

import jax
import jax.numpy as jnp
from jax import lax
from jax.experimental import pallas as pl
from jax.experimental.pallas import tpu as pltpu
from jax.sharding import PartitionSpec as P

momentum_decay = 0.9
moment_decay = 0.95
clip_level = 0.25
step_rate = 0.1
MESH = pl.DeviceIdType.MESH
LANES = 128


def chunk_rows(height):
    return LANES if height % LANES == 0 else height


def fold(x):
    return jnp.sum(x.reshape(x.shape[0] // 8, 8, x.shape[1]), axis=0)


def to_lanes(x):
    rows = x.shape[0]
    if rows < LANES:
        x = jnp.concatenate([x, jnp.zeros((LANES - rows, LANES), x.dtype)], axis=0)
    return jnp.sum(x.T, axis=0, keepdims=True)


def to_rows(x, rows):
    return jnp.broadcast_to(x, (LANES, LANES)).T[:rows]


def gather_kernel(sizes, n_fs, n_tp, *refs):
    n_all = n_fs * n_tp
    ins, refs = refs[:20], refs[20:]
    outs, refs = refs[:20], refs[20:]
    own, refs = refs[:4], refs[4:]
    other, refs = refs[:4], refs[4:]
    row_all, refs = refs[:4], refs[4:]
    column_part, refs = refs[:4], refs[4:]
    column_all, refs = refs[:4], refs[4:]
    share_all, refs = refs[:4], refs[4:]
    (own_sem, other_send, other_recv, momentum_sem, weight_sem,
     row_send, row_recv, column_send, column_recv, share_send, share_recv) = refs
    fs, tp, rep = lax.axis_index("fs"), lax.axis_index("tp"), lax.axis_index("rep")
    me = fs * n_tp + tp
    barrier = pltpu.get_barrier_semaphore()

    def place(d):
        lin = lax.rem(me + d, n_all)
        return {"fs": lax.div(lin, n_tp), "tp": lax.rem(lin, n_tp)}

    pl.semaphore_signal(barrier, inc=1, device_id={"rep": 1 - rep}, device_id_type=MESH)

    @pl.loop(1, n_all)
    def _(d):
        pl.semaphore_signal(barrier, inc=1, device_id=place(d), device_id_type=MESH)

    base = [0]
    for height, width in sizes:
        base.append(base[-1] + height // chunk_rows(height))

    def span(k, c):
        rows = chunk_rows(sizes[k][0])
        return pl.ds(pl.multiple_of(c * rows, rows), rows)

    def load(k, c):
        return pltpu.make_async_copy(
            ins[5 * k + 2].at[0, span(k, c)], own[k].at[span(k, c)], own_sem.at[base[k] + c])

    def send(k, c):
        return pltpu.make_async_remote_copy(
            src_ref=ins[5 * k + 2].at[0, span(k, c)], dst_ref=other[k].at[span(k, c)],
            send_sem=other_send.at[base[k] + c], recv_sem=other_recv.at[base[k] + c],
            device_id={"rep": 1 - rep}, device_id_type=MESH)

    def load_momentum(k, c):
        return pltpu.make_async_copy(
            ins[5 * k + 1].at[span(k, c)], outs[5 * k + 1].at[span(k, c)], momentum_sem.at[base[k] + c])

    def load_weight(k):
        return pltpu.make_async_copy(ins[5 * k], outs[5 * k], weight_sem.at[k])

    def each(k, f):
        @pl.loop(0, base[k + 1] - base[k])
        def _(c):
            f(k, c)

    each(0, lambda k, c: load(k, c).start())
    each(0, lambda k, c: load_momentum(k, c).start())
    pl.semaphore_wait(barrier, n_all)
    for k in range(4):
        each(k, lambda k, c: send(k, c).start())
    for k in range(1, 4):
        each(k, lambda k, c: load(k, c).start())
        each(k, lambda k, c: load_momentum(k, c).start())
    for k in range(4):
        load_weight(k).start()

    def accumulate(k):
        height, width = sizes[k]
        rows, tiles = chunk_rows(height), width // LANES
        column_part[k][...] = jnp.zeros_like(column_part[k])

        @pl.loop(0, height // rows)
        def _(c):
            load(k, c).wait()
            load_momentum(k, c).wait()
            send(k, c).wait_recv()
            part = jnp.zeros((rows, LANES), jnp.float32)
            for j in range(tiles):
                at = (span(k, c), pl.ds(j * LANES, LANES))
                grad = own[k][at] + other[k][at]
                outs[5 * k + 1][at] = momentum_decay * outs[5 * k + 1][at] + (1.0 - momentum_decay) * grad
                square = grad * grad
                part = part + square
                column_part[k][:, pl.ds(j * LANES, LANES)] += fold(square)
            row_all[k][tp, pl.ds(c, 1)] = to_lanes(part)

        column_all[k][fs] = jnp.sum(column_part[k][...], axis=0, keepdims=True)

    def row_copy(k, d):
        peer = lax.rem(tp + d, n_tp)
        return pltpu.make_async_remote_copy(
            src_ref=row_all[k].at[tp], dst_ref=row_all[k].at[tp],
            send_sem=row_send.at[k, d], recv_sem=row_recv.at[k, d],
            device_id={"tp": peer}, device_id_type=MESH)

    def column_copy(k, d):
        peer = lax.rem(fs + d, n_fs)
        return pltpu.make_async_remote_copy(
            src_ref=column_all[k].at[fs], dst_ref=column_all[k].at[fs],
            send_sem=column_send.at[k, d], recv_sem=column_recv.at[k, d],
            device_id={"fs": peer}, device_id_type=MESH)

    def share_copy(k, d):
        return pltpu.make_async_remote_copy(
            src_ref=share_all[k].at[me], dst_ref=share_all[k].at[me],
            send_sem=share_send.at[k, d], recv_sem=share_recv.at[k, d],
            device_id=place(d), device_id_type=MESH)

    def send_sums(k):
        @pl.loop(1, n_fs)
        def _(d):
            column_copy(k, d).start()

        @pl.loop(1, n_tp)
        def _(d):
            row_copy(k, d).start()

    def moments(k):
        height, width = sizes[k]
        rows, tiles = chunk_rows(height), width // LANES

        @pl.loop(1, n_tp)
        def _(d):
            row_copy(k, d).wait_recv()

        @pl.loop(1, n_fs)
        def _(d):
            column_copy(k, d).wait_recv()

        row_total = jnp.sum(row_all[k][...], axis=0) / (width * n_tp)
        row_next = moment_decay * ins[5 * k + 3][...] + (1.0 - moment_decay) * row_total
        outs[5 * k + 2][...] = row_next
        column_total = jnp.sum(column_all[k][...], axis=0) / (height * n_fs)
        column_next = moment_decay * ins[5 * k + 4][...] + (1.0 - moment_decay) * column_total
        outs[5 * k + 3][...] = column_next
        lane = lax.broadcasted_iota(jnp.int32, row_next.shape, 1)
        mass = jnp.sum(jnp.where(lane < rows, row_next, 0.0), axis=0, keepdims=True)

        def step(c, sums):
            inverse = to_rows(1.0 / outs[5 * k + 2][pl.ds(c, 1)], rows)
            new = []
            for j in range(tiles):
                m = outs[5 * k + 1][span(k, c), pl.ds(j * LANES, LANES)]
                new.append(sums[j] + fold(m * m * inverse))
            return tuple(new)

        zero = jnp.zeros((8, LANES), jnp.float32)
        sums = lax.fori_loop(0, height // rows, step, (zero,) * tiles)
        share = zero
        for j in range(tiles):
            share = share + sums[j] / outs[5 * k + 3][:, pl.ds(j * LANES, LANES)]
        share = jnp.sum(share, axis=0, keepdims=True)
        share_all[k][me] = jnp.concatenate([share, mass], axis=0)

    def send_share(k):
        @pl.loop(1, n_all)
        def _(d):
            share_copy(k, d).start()

    def scale(k):
        height, width = sizes[k]

        @pl.loop(1, n_all)
        def _(d):
            share_copy(k, d).wait_recv()

        total = jnp.sum(share_all[k][...], axis=0)
        total = jnp.sum(total, axis=1, keepdims=True)
        row_mean = total[1:2] / (height * n_fs * n_tp)
        spread = jnp.sqrt(row_mean * total[0:1] / (height * n_fs * width * n_tp))
        factor = jnp.maximum(1.0, spread / clip_level)
        outs[5 * k + 4][...] = jnp.broadcast_to(step_rate * jnp.sqrt(row_mean) / factor, (1, LANES))

    for k in range(4):
        accumulate(k)
        send_sums(k)
        if k >= 1:
            moments(k - 1)
            send_share(k - 1)
        if k >= 2:
            scale(k - 2)
    moments(3)
    send_share(3)
    scale(2)
    scale(3)
    for k in range(4):
        load_weight(k).wait()
        each(k, lambda k, c: send(k, c).wait_send())

        @pl.loop(1, n_tp)
        def _(d):
            row_copy(k, d).wait_send()

        @pl.loop(1, n_fs)
        def _(d):
            column_copy(k, d).wait_send()

        @pl.loop(1, n_all)
        def _(d):
            share_copy(k, d).wait_send()


def write_kernel(sizes, *refs):
    ins, refs = refs[:20], refs[20:]
    outs, refs = refs[:16], refs[16:]
    weight_next, refs = refs[:4], refs[4:]
    momentum_sem, weight_sem = refs

    def put_momentum(k):
        return pltpu.make_async_copy(ins[5 * k + 1], outs[4 * k + 1], momentum_sem.at[k])

    base = [0]
    for height, width in sizes:
        base.append(base[-1] + height // chunk_rows(height))

    def span(k, c):
        rows = chunk_rows(sizes[k][0])
        return pl.ds(pl.multiple_of(c * rows, rows), rows)

    def put_weight(k, c):
        return pltpu.make_async_copy(
            weight_next[k].at[span(k, c)], outs[4 * k].at[span(k, c)], weight_sem.at[base[k] + c])

    for k in range(4):
        put_momentum(k).start()
    for k, (height, width) in enumerate(sizes):
        rows = chunk_rows(height)
        outs[4 * k + 2][...] = ins[5 * k + 2][:, :rows]
        outs[4 * k + 3][...] = ins[5 * k + 3][...]

        @pl.loop(0, height // rows)
        def _(c):
            row_factor = to_rows(lax.rsqrt(ins[5 * k + 2][pl.ds(c, 1)]), rows)
            for j in range(width // LANES):
                at = (span(k, c), pl.ds(j * LANES, LANES))
                column_factor = lax.rsqrt(ins[5 * k + 3][:, pl.ds(j * LANES, LANES)]) * ins[5 * k + 4][...]
                weight_next[k][at] = ins[5 * k][at] - ins[5 * k + 1][at] * row_factor * column_factor
            put_weight(k, c).start()

    for k, (height, width) in enumerate(sizes):
        put_momentum(k).wait()

        @pl.loop(0, height // chunk_rows(height))
        def _(c):
            put_weight(k, c).wait()


def body(n_fs, n_tp, *arrays):
    f32 = jnp.float32
    sizes = tuple(arrays[5 * k].shape for k in range(4))
    chunks = [height // chunk_rows(height) for height, _ in sizes]
    n_all, total = n_fs * n_tp, sum(chunks)
    operands, middle = [], []
    in_specs = []
    hbm, vmem = pl.BlockSpec(memory_space=pl.ANY), pl.BlockSpec(memory_space=pltpu.VMEM)
    for k, (height, width) in enumerate(sizes):
        w, m, g, r, c = arrays[5 * k:5 * k + 5]
        rows = chunk_rows(height)
        r = r.reshape(chunks[k], rows)
        if rows < LANES:
            r = jnp.pad(r, ((0, 0), (0, LANES - rows)), constant_values=1.0)
        operands += [w, m, g, r, c.reshape(1, width)]
        in_specs += [hbm, hbm, hbm, vmem, vmem]
        middle += [pltpu.VMEM((height, width), f32), pltpu.VMEM((height, width), f32),
                   pltpu.VMEM((chunks[k], LANES), f32), pltpu.VMEM((1, width), f32), pltpu.VMEM((1, LANES), f32)]
    scratch = [pltpu.VMEM(s, f32) for s in sizes] + [pltpu.VMEM(s, f32) for s in sizes]
    scratch += [pltpu.VMEM((n_tp, n, LANES), f32) for n in chunks]
    scratch += [pltpu.VMEM((8, s[1]), f32) for s in sizes]
    scratch += [pltpu.VMEM((n_fs, 1, s[1]), f32) for s in sizes]
    scratch += [pltpu.VMEM((n_all, 2, LANES), f32) for s in sizes]
    dma = pltpu.SemaphoreType.DMA
    scratch += [dma((total,)), dma((total,)), dma((total,)), dma((total,)), dma((4,))]
    scratch += [dma((4, n_tp)), dma((4, n_tp)), dma((4, n_fs)), dma((4, n_fs)), dma((4, n_all)), dma((4, n_all))]
    block = 4 * sum(h * w for h, w in sizes)
    slack = 4 << 20
    middle = pl.pallas_call(
        functools.partial(gather_kernel, sizes, n_fs, n_tp),
        out_shape=middle,
        in_specs=in_specs,
        out_specs=[vmem] * 20,
        scratch_shapes=scratch,
        compiler_params=pltpu.CompilerParams(
            collective_id=0, has_side_effects=True, vmem_limit_bytes=2 * block + slack),
        name="gather",
    )(*operands)
    out_shape, out_specs = [], []
    for k, (height, width) in enumerate(sizes):
        rows = chunk_rows(height)
        out_shape += [jax.ShapeDtypeStruct((height, width), f32)] * 2
        out_shape += [jax.ShapeDtypeStruct((chunks[k], rows), f32), jax.ShapeDtypeStruct((1, width), f32)]
        out_specs += [hbm, hbm, vmem, vmem]
    outs = pl.pallas_call(
        functools.partial(write_kernel, sizes),
        out_shape=out_shape,
        in_specs=[vmem] * 20,
        out_specs=out_specs,
        scratch_shapes=[pltpu.VMEM(s, f32) for s in sizes] + [dma((4,)), dma((total,))],
        compiler_params=pltpu.CompilerParams(vmem_limit_bytes=block + slack),
        name="write",
    )(*middle)
    results = []
    for k in range(4):
        results += [outs[4 * k], outs[4 * k + 1], outs[4 * k + 2].reshape(-1), outs[4 * k + 3].reshape(-1)]
    return tuple(results)


def solution(mesh):
    matrix, partial, row, column = P("fs", "tp"), P("rep", "fs", "tp"), P("fs"), P("tp")
    return jax.shard_map(
        functools.partial(body, mesh.shape["fs"], mesh.shape["tp"]),
        mesh=mesh,
        in_specs=(matrix, matrix, partial, row, column) * 4,
        out_specs=(matrix, matrix, row, column) * 4,
        check_vma=False,
    )
```
